32 devices in a mesh: kv: 8 (over y, x, core), tp: 4 (over z).
Axes of the slice: x: 2, y: 2, z: 4, core: 2. Of those that a mesh axis runs over, the one named last changes fastest.
Arguments:
- tokens: bfloat16 [320, 4096], P('tp', 'kv'), may hold values from -8 to 8
- state: float32 [320, 32, 128, 128], P('kv', 'tp'), may hold values from -4 to 4
- mix_gain: float32 [4096], P('kv'), may hold values from 0.1 to 1.9
- q_weight: bfloat16 [4096, 4096], P('kv', 'tp'), may hold values from -0.09375 to 0.09375
- forget_weight: bfloat16 [4096, 4096], P('kv', 'tp'), may hold values from -0.09375 to 0.09375
- input_weight: bfloat16 [4096, 4096], P('kv', 'tp'), may hold values from -0.09375 to 0.09375
- gate_weight: bfloat16 [4096, 4096], P('kv', 'tp'), may hold values from -0.09375 to 0.09375
- lower_bound: float32 [4096], P('tp'), may hold values from 0 to 0.9
- head_gain: float32 [128], replicated, may hold values from 0.1 to 1.9
- out_weight: bfloat16 [4096, 4096], P('tp', 'kv'), may hold values from -0.09375 to 0.09375
- ffn_gain: float32 [4096], P('kv'), may hold values from 0.1 to 1.9
- ffn_gate: bfloat16 [4096, 10240], P('kv', 'tp'), may hold values from -0.09375 to 0.09375
- ffn_up: bfloat16 [4096, 10240], P('kv', 'tp'), may hold values from -0.09375 to 0.09375
- ffn_down: bfloat16 [10240, 4096], P('tp', 'kv'), may hold values from -0.0625 to 0.0625
Outputs:
- layer_out: bfloat16 [320, 4096], P('tp', 'kv')
- new_state: float32 [320, 32, 128, 128], P('kv', 'tp')
The draws below stay inside these ranges and needn't reach their ends.
All inputs are finite; a program needn't handle non-finite values.
Results may differ from the reference program's by a relative error of at most 0.007.
Values may be sent and summed in bfloat16 or wider, within the bound.
A program may use at most 128 MiB of HBM per device.

```python
import jax
import jax.numpy as jnp
from jax import lax

HEADS = 32
HEAD = 128
D = 4096
FF = 10240
BATCH = 320


def draw_tokens(key, part):
    first, second, third, fourth = jax.random.split(jax.random.fold_in(key, 17), 4)
    base = jax.random.normal(first, (BATCH, D), jnp.float32)
    block_scale = jnp.exp(jax.random.uniform(second, (32,), jnp.float32, -1.2, 1.2))
    column_scale = jnp.repeat(block_scale, D // 32)
    values = base * column_scale[None, :]
    return jnp.clip(values, -8.0, 8.0).astype(jnp.bfloat16)


def levels(stream_key, shape, cuts, least, top_value):
    def one(axis_at, parts):
        draws = jax.random.uniform(jax.random.fold_in(jax.random.fold_in(stream_key, 6), axis_at), (parts,), jnp.float32, least / len(cuts), top_value / len(cuts))
        return jnp.repeat(jnp.exp(draws), shape[axis_at] // parts).reshape((-1,) + (1,) * (len(shape) - axis_at - 1))

    loudness = one(*cuts[0])
    for cut in cuts[1:]:
        loudness = loudness * one(*cut)
    return loudness


def gaussian(key, shape, scale, bound, shards=(), kind=jnp.bfloat16):
    array = scale * jax.random.normal(key, shape, jnp.float32)
    if shards:
        array = array * levels(key, shape, shards, -0.22, 0.18)
    return jnp.clip(array, -bound, bound).astype(kind)


def setup_inputs(seed: int = 0) -> dict:
    key_of = jax.random.split(jax.random.key(seed), 15)
    tokens = draw_tokens(jax.random.fold_in(key_of[14], 71), 0)
    state = gaussian(key_of[1], (BATCH, HEADS, HEAD, HEAD), 0.5, 4.0, ((0, 8), (1, 4)), jnp.float32)
    mix_gain = jnp.clip(1.0 + 0.18 * jax.random.normal(key_of[2], (D,), jnp.float32), 0.1, 1.9)
    q_weight = gaussian(key_of[3], (D, D), D ** -0.5, 0.09375, ((0, 8), (1, 4)))
    forget_weight = gaussian(key_of[4], (D, D), D ** -0.5, 0.09375, ((0, 8), (1, 4)))
    input_weight = gaussian(key_of[5], (D, D), D ** -0.5, 0.09375, ((0, 8), (1, 4)))
    gate_weight = gaussian(key_of[6], (D, D), D ** -0.5, 0.09375, ((0, 8), (1, 4)))
    lower_bound = jnp.clip(0.9 * jax.random.uniform(key_of[7], (D,), jnp.float32) ** levels(key_of[7], (D,), ((0, 4),), -0.2, 0.2), 0.0, 0.9)
    head_gain = jnp.clip(1.0 + 0.18 * jax.random.normal(key_of[8], (HEAD,), jnp.float32), 0.1, 1.9)
    out_weight = gaussian(key_of[9], (D, D), D ** -0.5, 0.09375, ((0, 4), (1, 8)))
    ffn_gain = jnp.clip(1.0 + 0.18 * jax.random.normal(key_of[10], (D,), jnp.float32), 0.1, 1.9)
    ffn_gate = gaussian(key_of[11], (D, FF), D ** -0.5, 0.09375, ((0, 8), (1, 4)))
    ffn_up = gaussian(key_of[12], (D, FF), D ** -0.5, 0.09375, ((0, 8), (1, 4)))
    ffn_down = gaussian(key_of[13], (FF, D), FF ** -0.5, 0.0625, ((0, 4), (1, 8)))
    return {"tokens": tokens, "state": state, "mix_gain": mix_gain, "q_weight": q_weight, "forget_weight": forget_weight, "input_weight": input_weight, "gate_weight": gate_weight, "lower_bound": lower_bound, "head_gain": head_gain, "out_weight": out_weight, "ffn_gain": ffn_gain, "ffn_gate": ffn_gate, "ffn_up": ffn_up, "ffn_down": ffn_down}


EPS = 1e-05

def reference(tokens, state, mix_gain, q_weight, forget_weight, input_weight, gate_weight, lower_bound, head_gain, out_weight, ffn_gain, ffn_gate, ffn_up, ffn_down):
    batch_rows = tokens.shape[0]
    values = tokens.astype(jnp.float32)
    factor = lax.rsqrt(lax.optimization_barrier(jnp.mean(values * values, axis=1, keepdims=True)) + EPS)
    normed = (values * mix_gain).astype(jnp.bfloat16)

    def project(weight):
        return jnp.dot(normed, weight, preferred_element_type=jnp.float32) * factor
    query_pre = project(q_weight)
    forget_pre = project(forget_weight)
    value_pre = project(input_weight)
    gate_pre = project(gate_weight)
    split_shape = (batch_rows, HEADS, HEAD)
    query = (jax.nn.silu(query_pre) * HEAD ** (-0.5)).reshape(split_shape)
    forget = (lower_bound + (1.0 - lower_bound) * jax.nn.sigmoid(forget_pre)).reshape(split_shape)
    value = value_pre.reshape(split_shape)
    new_state = forget[..., None] * state + (1.0 - forget)[..., None] * value[:, :, None, :]
    read = jnp.einsum('bhk,bhkv->bhv', query, new_state, precision=lax.Precision.HIGHEST)
    read = read * lax.rsqrt(lax.optimization_barrier(jnp.mean(read * read, axis=-1, keepdims=True)) + EPS) * head_gain
    gated = (read.reshape(batch_rows, D) * jax.nn.silu(gate_pre)).astype(jnp.bfloat16)
    residual = (values + jnp.dot(gated, out_weight, preferred_element_type=jnp.float32)).astype(jnp.bfloat16)
    res_values = residual.astype(jnp.float32)
    factor_ffn = lax.rsqrt(lax.optimization_barrier(jnp.mean(res_values * res_values, axis=1, keepdims=True)) + EPS)
    normed_ffn = (res_values * ffn_gain).astype(jnp.bfloat16)
    gate_ffn = jnp.dot(normed_ffn, ffn_gate, preferred_element_type=jnp.float32) * factor_ffn
    up_ffn = jnp.dot(normed_ffn, ffn_up, preferred_element_type=jnp.float32) * factor_ffn
    hidden = (jax.nn.silu(gate_ffn) * up_ffn).astype(jnp.bfloat16)
    layer_out = (res_values + jnp.dot(hidden, ffn_down, preferred_element_type=jnp.float32)).astype(jnp.bfloat16)
    return (layer_out, new_state)
```

```python
import functools

import jax
import jax.numpy as jnp
from jax import lax
from jax.experimental import pallas as pl
from jax.experimental.pallas import tpu as pltpu
from jax.sharding import PartitionSpec as P

EPS = 1e-05
F32 = jnp.float32
BF16 = jnp.bfloat16
LANES = 128
MESH = pl.DeviceIdType.MESH
ANY = pl.BlockSpec(memory_space=pl.ANY)
VMEM = pl.BlockSpec(memory_space=pltpu.VMEM)


def remote(src, dst, send, recv, axis, peer):
    return pltpu.make_async_remote_copy(
        src_ref=src,
        dst_ref=dst,
        send_sem=send,
        recv_sem=recv,
        device_id={axis: peer},
        device_id_type=MESH,
    )


def greet(n_kv, n_tp):
    kv, tp = lax.axis_index("kv"), lax.axis_index("tp")
    barrier = pltpu.get_barrier_semaphore()
    for axis, me, n in (("kv", kv, n_kv), ("tp", tp, n_tp)):
        for off in range(1, n):
            pl.semaphore_signal(
                barrier,
                inc=1,
                device_id={axis: lax.rem(me + off, n)},
                device_id_type=MESH,
            )
    pl.semaphore_wait(barrier, n_kv + n_tp - 2)


def partner_of(me):
    return me + 1 - 2 * lax.rem(me, 2)


def exchange_start(src_at, dst, send, recv, axis, n):
    me = lax.axis_index(axis)
    copies = []
    for off in range(1, n):
        peer = lax.rem(me + off, n)
        copy = remote(src_at(peer), dst.at[me], send.at[off], recv.at[off], axis, peer)
        copy.start()
        copies.append(copy)
    return copies


def gather_kv(own, gathered, send, recv, fsend, frecv, n):
    me = lax.axis_index("kv")
    half = n // 2
    mine = me // 2
    parity = lax.rem(me, 2)
    partner = partner_of(me)
    first = []
    for off in range(1, half):
        peer = lax.rem(mine + off, half) * 2 + parity
        copy = remote(own, gathered.at[me], send.at[off], recv.at[off], "kv", peer)
        copy.start()
        first.append(copy)
    pair = remote(own, gathered.at[me], fsend.at[0], frecv.at[0], "kv", partner)
    pair.start()
    gathered[me] = own[...]
    second = [pair]
    for off in range(1, half):
        first[off - 1].wait_recv()
        source = lax.rem(mine + half - off, half) * 2 + parity
        copy = remote(
            gathered.at[source], gathered.at[source], fsend.at[off], frecv.at[off], "kv", partner
        )
        copy.start()
        second.append(copy)
    for copy in second:
        copy.wait_recv()
    return first + second


class Scatter:
    def __init__(self, refs, n):
        (self.out, self.pair_in, self.mid, self.rest_in, self.ps, self.pr, self.rs, self.rr) = refs
        self.n = n
        self.half = n // 2
        self.me = lax.axis_index("kv")
        self.mine = self.me // 2
        self.parity = lax.rem(self.me, 2)
        self.pairs = []
        self.rests = []

    def put(self, c, cols, block):
        rows = block.shape[0] // self.n
        for j in range(self.n):
            self.out[c, j % 2, j // 2, :, cols] = block[j * rows : (j + 1) * rows].astype(BF16)

    def send_pair(self, c):
        copy = remote(
            self.out.at[c, 1 - self.parity],
            self.pair_in.at[c],
            self.ps.at[c],
            self.pr.at[c],
            "kv",
            partner_of(self.me),
        )
        copy.start()
        self.pairs.append(copy)

    def pair_sum(self, c, j):
        return self.out[c, self.parity, j].astype(F32) + self.pair_in[c, j].astype(F32)

    def send_rest(self, c):
        self.pairs[c].wait_recv()
        copies = []
        for off in range(1, self.half):
            j = lax.rem(self.mine + off, self.half)
            self.mid[c, off] = self.pair_sum(c, j).astype(BF16)
            copy = remote(
                self.mid.at[c, off],
                self.rest_in.at[c, off],
                self.rs.at[c, off],
                self.rr.at[c, off],
                "kv",
                j * 2 + self.parity,
            )
            copy.start()
            copies.append(copy)
        self.rests.append(copies)

    def total(self, c):
        for copy in self.rests[c]:
            copy.wait_recv()
        total = self.pair_sum(c, self.mine)
        for off in range(1, self.half):
            total = total + self.rest_in[c, off].astype(F32)
        return total

    def close(self):
        for copy in self.pairs:
            copy.wait_send()
        for copies in self.rests:
            for copy in copies:
                copy.wait_send()


def scatter_scratch(chunks, n, rows, cols):
    half = n // 2
    return [
        pltpu.VMEM((chunks, 2, half, rows, cols), BF16),
        pltpu.VMEM((chunks, half, rows, cols), BF16),
        pltpu.VMEM((chunks, half, rows, cols), BF16),
        pltpu.VMEM((chunks, half, rows, cols), BF16),
        pltpu.SemaphoreType.DMA((chunks,)),
        pltpu.SemaphoreType.DMA((chunks,)),
        pltpu.SemaphoreType.DMA((chunks, half)),
        pltpu.SemaphoreType.DMA((chunks, half)),
    ]


def squares_scratch(n, rows):
    return [
        pltpu.VMEM((n, rows, LANES), F32),
        pltpu.VMEM((n, rows, LANES), F32),
        pltpu.SemaphoreType.DMA((n,)),
        pltpu.SemaphoreType.DMA((n,)),
    ]


def squares_start(values, refs, n):
    out, into, send, recv = refs
    totals = jnp.sum(values * values, axis=1, keepdims=True)
    totals = jnp.broadcast_to(totals, (values.shape[0], LANES))
    out[...] = totals.reshape(out.shape)
    return exchange_start(lambda peer: out.at[peer], into, send, recv, "kv", n)


def squares_factor(copies, refs, n, width):
    out, into, _, _ = refs
    me = lax.axis_index("kv")
    for copy in copies:
        copy.wait_recv()
    total = out[me]
    for off in range(1, n):
        total = total + into[lax.rem(me + off, n)]
    return lax.rsqrt(total[:, :1] / width + EPS)


def tile_of(cols):
    return 512 if cols % 512 == 0 else cols


def mixer_in(n_kv, n_tp, width, tokens, gain, wq, wf, wv, wg, sums, rows_all, weights, *rest):
    scatter_refs, square_refs = rest[:8], rest[8:12]
    load_sem, t_send, t_recv = rest[12:]
    tp = lax.axis_index("tp")
    loads = [
        pltpu.make_async_copy(w, weights.at[i], load_sem.at[i])
        for i, w in enumerate((wq, wf, wv, wg))
    ]
    for load in loads:
        load.start()
    greet(n_kv, n_tp)
    copies = exchange_start(lambda peer: tokens, rows_all, t_send, t_recv, "tp", n_tp)
    rows_all[tp] = tokens[...]
    for copy in copies:
        copy.wait_recv()
    batch = n_tp * tokens.shape[0]
    values = rows_all[...].astype(F32).reshape(batch, tokens.shape[1])
    normed = (values * gain[...]).astype(BF16)
    scatter = Scatter(scatter_refs, n_kv)
    cols = weights.shape[2]
    tile = tile_of(cols)
    squares = None
    for c in range(4):
        loads[c].wait()
        for at in range(0, cols, tile):
            part = pl.ds(at, tile)
            scatter.put(
                c, part, jnp.dot(normed, weights[c, :, part], preferred_element_type=F32)
            )
        scatter.send_pair(c)
        if c > 0:
            scatter.send_rest(c - 1)
        if c == 0:
            squares = squares_start(values, square_refs, n_kv)
    scatter.send_rest(3)
    factor = squares_factor(squares, square_refs, n_kv, width)
    for c in range(4):
        sums[:, c * cols : (c + 1) * cols] = scatter.total(c) * factor
    for copy in copies + squares:
        copy.wait_send()
    scatter.close()


def state_step(q_pre, f_pre, v_pre, g_pre, bound, head_gain, state, new_state, gated, read):
    rows = q_pre.shape[0]
    size = state.shape[-1]
    low = bound[...]
    query = jax.nn.silu(q_pre[...]) * size ** (-0.5)
    forget = low + (1.0 - low) * jax.nn.sigmoid(f_pre[...])
    query_t = query.T
    forget_t = forget.T
    value = v_pre[...]
    for b in range(rows):
        v = value[b : b + 1, :]
        new = v + forget_t[:, b : b + 1] * (state[b, 0] - v)
        new_state[b, 0] = new
        read[b : b + 1, :] = jnp.sum(query_t[:, b : b + 1] * new, axis=0, keepdims=True)
    out = read[...]
    out = out * lax.rsqrt(jnp.mean(out * out, axis=1, keepdims=True) + EPS) * head_gain[...]
    gated[...] = (out * jax.nn.silu(g_pre[...])).astype(BF16)


def rest_of_layer(
    n_kv, n_tp, width, chunks, tokens, gated, gain, w_out, w_gate, w_up, w_down, out, *refs
):
    (v_out, v_ffn, v_down, g_all, h_own, h_all, t_acc, t_send_buf, t_recv_buf, r_own, r_all) = refs[:11]
    scatter_refs, square_refs = refs[11:19], refs[19:23]
    (load_sem, gs, gr, gfs, gfr, hs, hr, hfs, hfr, ts, tr) = refs[23:]
    tp = lax.axis_index("tp")
    loads = [
        pltpu.make_async_copy(w_out, v_out, load_sem.at[0]),
        pltpu.make_async_copy(w_gate, v_ffn.at[0], load_sem.at[1]),
        pltpu.make_async_copy(w_up, v_ffn.at[1], load_sem.at[2]),
        pltpu.make_async_copy(w_down, v_down, load_sem.at[3]),
    ]
    for load in loads:
        load.start()
    greet(n_kv, n_tp)
    done = []
    rows_tp = tokens.shape[0]

    def sum_tp(k, left, right):
        batch = n_tp * rows_tp
        values = left[...].astype(F32).reshape(batch, left.shape[2]).astype(BF16)
        product = jnp.dot(values, right[...], preferred_element_type=F32)
        product = product.reshape(n_tp, rows_tp, product.shape[1])
        t_acc[...] = product
        t_send_buf[k] = product.astype(BF16)
        copies = exchange_start(
            lambda peer: t_send_buf.at[k, peer], t_recv_buf.at[k], ts.at[k], tr.at[k], "tp", n_tp
        )
        total = t_acc[tp]
        for off in range(1, n_tp):
            copies[off - 1].wait_recv()
            total = total + t_recv_buf[k, lax.rem(tp + n_tp - off, n_tp)].astype(F32)
        done.extend(copies)
        return total

    done.extend(gather_kv(gated, g_all, gs, gr, gfs, gfr, n_kv))
    loads[0].wait()
    attended = sum_tp(0, g_all, v_out)
    r_own[...] = (tokens[...].astype(F32) + attended).astype(BF16)
    copies = exchange_start(lambda peer: r_own, r_all, ts.at[2], tr.at[2], "tp", n_tp)
    r_all[tp] = r_own[...]
    for copy in copies:
        copy.wait_recv()
    done.extend(copies)
    values = r_all[...].astype(F32).reshape(n_tp * rows_tp, tokens.shape[1])
    normed = (values * gain[...]).astype(BF16)
    scatter = Scatter(scatter_refs, n_kv)
    cols = v_ffn.shape[2]
    step = cols // chunks
    tile = next(t for t in (640, 512, 256, 128) if step % t == 0)
    order = [(w, h) for h in range(chunks) for w in range(2)]
    loads[1].wait()
    loads[2].wait()
    squares = None
    for c, (w, h) in enumerate(order):
        for at in range(0, step, tile):
            product = jnp.dot(
                normed, v_ffn[w, :, pl.ds(h * step + at, tile)], preferred_element_type=F32
            )
            scatter.put(c, pl.ds(at, tile), product)
        scatter.send_pair(c)
        if c > 0:
            scatter.send_rest(c - 1)
        if c == 0:
            squares = squares_start(values, square_refs, n_kv)
    scatter.send_rest(2 * chunks - 1)
    factor = squares_factor(squares, square_refs, n_kv, width)
    done.extend(squares)
    for h in range(chunks):
        gate = scatter.total(2 * h) * factor
        up = scatter.total(2 * h + 1) * factor
        h_own[:, h * step : (h + 1) * step] = (jax.nn.silu(gate) * up).astype(BF16)
    done.extend(gather_kv(h_own, h_all, hs, hr, hfs, hfr, n_kv))
    loads[3].wait()
    down = sum_tp(1, h_all, v_down)
    out[...] = (r_own[...].astype(F32) + down).astype(BF16)
    for copy in done:
        copy.wait_send()
    scatter.close()


def body(
    n_kv,
    n_tp,
    tokens,
    state,
    mix_gain,
    q_weight,
    forget_weight,
    input_weight,
    gate_weight,
    lower_bound,
    head_gain,
    out_weight,
    ffn_gain,
    ffn_gate,
    ffn_up,
    ffn_down,
):
    rows_tp, feats = tokens.shape
    width = feats * n_kv
    rows_kv, heads, size = state.shape[:3]
    cols = q_weight.shape[1]
    ff = ffn_gate.shape[1]
    dma = pltpu.SemaphoreType.DMA
    sums = pl.pallas_call(
        functools.partial(mixer_in, n_kv, n_tp, width),
        out_shape=jax.ShapeDtypeStruct((rows_kv, 4 * cols), F32),
        in_specs=[VMEM, VMEM, ANY, ANY, ANY, ANY],
        out_specs=VMEM,
        scratch_shapes=[
            pltpu.VMEM((n_tp, rows_tp, feats), BF16),
            pltpu.VMEM((4, feats, cols), BF16),
            *scatter_scratch(4, n_kv, rows_kv, cols),
            *squares_scratch(n_kv, rows_kv),
            dma((4,)),
            dma((n_tp,)),
            dma((n_tp,)),
        ],
        compiler_params=pltpu.CompilerParams(collective_id=0, has_side_effects=True),
        name="mixer_in",
    )(tokens, mix_gain[None, :], q_weight, forget_weight, input_weight, gate_weight)

    def part(i):
        return pl.BlockSpec((rows_kv, size), lambda h: (0, i * heads + h))

    state_block = pl.BlockSpec((rows_kv, 1, size, size), lambda h: (0, h, 0, 0))
    new_state, gated = pl.pallas_call(
        state_step,
        out_shape=(
            jax.ShapeDtypeStruct(state.shape, F32),
            jax.ShapeDtypeStruct((rows_kv, cols), BF16),
        ),
        grid=(heads,),
        in_specs=[
            part(0),
            part(1),
            part(2),
            part(3),
            pl.BlockSpec((1, size), lambda h: (0, h)),
            pl.BlockSpec((1, size), lambda h: (0, 0)),
            state_block,
        ],
        out_specs=(state_block, pl.BlockSpec((rows_kv, size), lambda h: (0, h))),
        scratch_shapes=[pltpu.VMEM((rows_kv, size), F32)],
        compiler_params=pltpu.CompilerParams(dimension_semantics=("arbitrary",)),
        name="state_step",
    )(sums, sums, sums, sums, lower_bound[None, :], head_gain[None, :], state)

    half = n_kv // 2
    chunks = 2 if ff % (2 * LANES) == 0 else 1
    layer_out = pl.pallas_call(
        functools.partial(rest_of_layer, n_kv, n_tp, width, chunks),
        out_shape=jax.ShapeDtypeStruct(tokens.shape, BF16),
        in_specs=[VMEM, VMEM, VMEM, ANY, ANY, ANY, ANY],
        out_specs=VMEM,
        scratch_shapes=[
            pltpu.VMEM((cols, feats), BF16),
            pltpu.VMEM((2, feats, ff), BF16),
            pltpu.VMEM((ff, feats), BF16),
            pltpu.VMEM((n_kv, rows_kv, cols), BF16),
            pltpu.VMEM((rows_kv, ff), BF16),
            pltpu.VMEM((n_kv, rows_kv, ff), BF16),
            pltpu.VMEM((n_tp, rows_tp, feats), F32),
            pltpu.VMEM((2, n_tp, rows_tp, feats), BF16),
            pltpu.VMEM((2, n_tp, rows_tp, feats), BF16),
            pltpu.VMEM((rows_tp, feats), BF16),
            pltpu.VMEM((n_tp, rows_tp, feats), BF16),
            *scatter_scratch(2 * chunks, n_kv, rows_kv, ff // chunks),
            *squares_scratch(n_kv, rows_kv),
            dma((4,)),
            *[dma((half,)) for _ in range(8)],
            dma((3, n_tp)),
            dma((3, n_tp)),
        ],
        compiler_params=pltpu.CompilerParams(collective_id=1, has_side_effects=True),
        name="rest_of_layer",
    )(tokens, gated, ffn_gain[None, :], out_weight, ffn_gate, ffn_up, ffn_down)
    return (layer_out, new_state)


def solution(mesh):
    in_specs = (
        P("tp", "kv"),
        P("kv", "tp", None, None),
        P("kv"),
        P("kv", "tp"),
        P("kv", "tp"),
        P("kv", "tp"),
        P("kv", "tp"),
        P("tp"),
        P(),
        P("tp", "kv"),
        P("kv"),
        P("kv", "tp"),
        P("kv", "tp"),
        P("tp", "kv"),
    )
    out_specs = (P("tp", "kv"), P("kv", "tp", None, None))
    step = functools.partial(body, mesh.shape["kv"], mesh.shape["tp"])
    return jax.shard_map(step, mesh=mesh, in_specs=in_specs, out_specs=out_specs, check_vma=False)
```

```python
import functools

import jax
import jax.numpy as jnp
from jax import lax
from jax.experimental import pallas as pl
from jax.experimental.pallas import tpu as pltpu
from jax.sharding import PartitionSpec as P

EPS = 1e-05
F32 = jnp.float32
BF16 = jnp.bfloat16
LANES = 128
MIB = 1 << 20
MESH = pl.DeviceIdType.MESH
HBM = pl.BlockSpec(memory_space=pltpu.HBM)
VMEM = pl.BlockSpec(memory_space=pltpu.VMEM)


def remote(src, dst, send, recv, axis, peer):
    return pltpu.make_async_remote_copy(
        src_ref=src,
        dst_ref=dst,
        send_sem=send,
        recv_sem=recv,
        device_id={axis: peer},
        device_id_type=MESH,
    )


def greet(n_kv, n_tp):
    kv, tp = lax.axis_index("kv"), lax.axis_index("tp")
    barrier = pltpu.get_barrier_semaphore()
    for axis, me, n in (("kv", kv, n_kv), ("tp", tp, n_tp)):
        for off in range(1, n):
            pl.semaphore_signal(
                barrier,
                inc=1,
                device_id={axis: lax.rem(me + off, n)},
                device_id_type=MESH,
            )
    pl.semaphore_wait(barrier, n_kv + n_tp - 2)


def partner_of(me):
    return me + 1 - 2 * lax.rem(me, 2)


def exchange_start(src_at, dst, send, recv, axis, n):
    me = lax.axis_index(axis)
    copies = []
    for off in range(1, n):
        peer = lax.rem(me + off, n)
        copy = remote(src_at(peer), dst.at[me], send.at[off], recv.at[off], axis, peer)
        copy.start()
        copies.append(copy)
    return copies


def gather_kv(own, gathered, send, recv, fsend, frecv, n):
    me = lax.axis_index("kv")
    half = n // 2
    mine = me // 2
    parity = lax.rem(me, 2)
    partner = partner_of(me)
    first = []
    for off in range(1, half):
        peer = lax.rem(mine + off, half) * 2 + parity
        copy = remote(own, gathered.at[me], send.at[off], recv.at[off], "kv", peer)
        copy.start()
        first.append(copy)
    pair = remote(own, gathered.at[me], fsend.at[0], frecv.at[0], "kv", partner)
    pair.start()
    gathered[me] = own[...]
    second = [pair]
    for off in range(1, half):
        first[off - 1].wait_recv()
        source = lax.rem(mine + half - off, half) * 2 + parity
        copy = remote(
            gathered.at[source], gathered.at[source], fsend.at[off], frecv.at[off], "kv", partner
        )
        copy.start()
        second.append(copy)
    for copy in second:
        copy.wait_recv()
    return first + second


class Scatter:
    def __init__(self, refs, n):
        (self.out, self.pair_in, self.mid, self.rest_in, self.ps, self.pr, self.rs, self.rr) = refs
        self.n = n
        self.half = n // 2
        self.me = lax.axis_index("kv")
        self.mine = self.me // 2
        self.parity = lax.rem(self.me, 2)
        self.pairs = []
        self.rests = []

    def put(self, c, cols, block):
        rows = block.shape[0] // self.n
        for j in range(self.n):
            self.out[c, j % 2, j // 2, :, cols] = block[j * rows : (j + 1) * rows].astype(BF16)

    def send_pair(self, c):
        copy = remote(
            self.out.at[c, 1 - self.parity],
            self.pair_in.at[c],
            self.ps.at[c],
            self.pr.at[c],
            "kv",
            partner_of(self.me),
        )
        copy.start()
        self.pairs.append(copy)

    def pair_sum(self, c, j):
        return self.out[c, self.parity, j].astype(F32) + self.pair_in[c, j].astype(F32)

    def send_rest(self, c):
        self.pairs[c].wait_recv()
        copies = []
        for off in range(1, self.half):
            j = lax.rem(self.mine + off, self.half)
            self.mid[c, off] = self.pair_sum(c, j).astype(BF16)
            copy = remote(
                self.mid.at[c, off],
                self.rest_in.at[c, off],
                self.rs.at[c, off],
                self.rr.at[c, off],
                "kv",
                j * 2 + self.parity,
            )
            copy.start()
            copies.append(copy)
        self.rests.append(copies)

    def total(self, c):
        for copy in self.rests[c]:
            copy.wait_recv()
        total = self.pair_sum(c, self.mine)
        for off in range(1, self.half):
            total = total + self.rest_in[c, off].astype(F32)
        return total

    def close(self):
        for copy in self.pairs:
            copy.wait_send()
        for copies in self.rests:
            for copy in copies:
                copy.wait_send()


def scatter_scratch(chunks, n, rows, cols):
    half = n // 2
    return [
        pltpu.VMEM((chunks, 2, half, rows, cols), BF16),
        pltpu.VMEM((chunks, half, rows, cols), BF16),
        pltpu.VMEM((chunks, half, rows, cols), BF16),
        pltpu.VMEM((chunks, half, rows, cols), BF16),
        pltpu.SemaphoreType.DMA((chunks,)),
        pltpu.SemaphoreType.DMA((chunks,)),
        pltpu.SemaphoreType.DMA((chunks, half)),
        pltpu.SemaphoreType.DMA((chunks, half)),
    ]


def squares_scratch(n, rows):
    return [
        pltpu.VMEM((n, rows, LANES), F32),
        pltpu.VMEM((n, rows, LANES), F32),
        pltpu.SemaphoreType.DMA((n,)),
        pltpu.SemaphoreType.DMA((n,)),
    ]


def squares_start(values, refs, n):
    out, into, send, recv = refs
    totals = jnp.sum(values * values, axis=1, keepdims=True)
    totals = jnp.broadcast_to(totals, (values.shape[0], LANES))
    out[...] = totals.reshape(out.shape)
    return exchange_start(lambda peer: out.at[peer], into, send, recv, "kv", n)


def squares_factor(copies, refs, n, width):
    out, into, _, _ = refs
    me = lax.axis_index("kv")
    for copy in copies:
        copy.wait_recv()
    total = out[me]
    for off in range(1, n):
        total = total + into[lax.rem(me + off, n)]
    return lax.rsqrt(total[:, :1] / width + EPS)


def tile_of(cols):
    return 512 if cols % 512 == 0 else cols


def mixer_in(n_kv, n_tp, width, tokens, gain, wq, wf, wv, wg, sums, rows_all, weights, *rest):
    scatter_refs, square_refs = rest[:8], rest[8:12]
    load_sem, t_send, t_recv = rest[12:]
    tp = lax.axis_index("tp")
    loads = [
        pltpu.make_async_copy(w, weights.at[i], load_sem.at[i])
        for i, w in enumerate((wq, wf, wv, wg))
    ]
    for load in loads:
        load.start()
    greet(n_kv, n_tp)
    copies = exchange_start(lambda peer: tokens, rows_all, t_send, t_recv, "tp", n_tp)
    rows_all[tp] = tokens[...]
    for copy in copies:
        copy.wait_recv()
    batch = n_tp * tokens.shape[0]
    values = rows_all[...].astype(F32).reshape(batch, tokens.shape[1])
    normed = (values * gain[...]).astype(BF16)
    scatter = Scatter(scatter_refs, n_kv)
    cols = weights.shape[2]
    tile = tile_of(cols)
    squares = None
    for c in range(4):
        loads[c].wait()
        for at in range(0, cols, tile):
            part = pl.ds(at, tile)
            scatter.put(
                c, part, jnp.dot(normed, weights[c, :, part], preferred_element_type=F32)
            )
        scatter.send_pair(c)
        if c > 0:
            scatter.send_rest(c - 1)
        if c == 0:
            squares = squares_start(values, square_refs, n_kv)
    scatter.send_rest(3)
    factor = squares_factor(squares, square_refs, n_kv, width)
    for c in range(4):
        sums[:, c * cols : (c + 1) * cols] = scatter.total(c) * factor
    for copy in copies + squares:
        copy.wait_send()
    scatter.close()


def state_step(q_pre, f_pre, v_pre, g_pre, bound, head_gain, state, new_state, gated, read):
    rows = q_pre.shape[0]
    size = state.shape[-1]
    low = bound[...]
    query = jax.nn.silu(q_pre[...]) * size ** (-0.5)
    forget = low + (1.0 - low) * jax.nn.sigmoid(f_pre[...])
    query_t = query.T
    forget_t = forget.T
    value = v_pre[...]
    for b in range(rows):
        v = value[b : b + 1, :]
        new = v + forget_t[:, b : b + 1] * (state[b, 0] - v)
        new_state[b, 0] = new
        read[b : b + 1, :] = jnp.sum(query_t[:, b : b + 1] * new, axis=0, keepdims=True)
    out = read[...]
    out = out * lax.rsqrt(jnp.mean(out * out, axis=1, keepdims=True) + EPS) * head_gain[...]
    gated[...] = (out * jax.nn.silu(g_pre[...])).astype(BF16)


def rest_of_layer(
    n_kv, n_tp, width, chunks, tokens, gated, gain, w_out, w_gate, w_up, w_down, out, *refs
):
    (v_out, v_ffn, v_down, g_all, h_own, h_all, t_acc, t_send_buf, t_recv_buf, r_own, r_all) = refs[:11]
    scatter_refs, square_refs = refs[11:19], refs[19:23]
    (load_sem, gs, gr, gfs, gfr, hs, hr, hfs, hfr, ts, tr) = refs[23:]
    tp = lax.axis_index("tp")
    loads = [
        pltpu.make_async_copy(w_out, v_out, load_sem.at[0]),
        pltpu.make_async_copy(w_gate, v_ffn.at[0], load_sem.at[1]),
        pltpu.make_async_copy(w_up, v_ffn.at[1], load_sem.at[2]),
        pltpu.make_async_copy(w_down, v_down, load_sem.at[3]),
    ]
    for load in loads:
        load.start()
    greet(n_kv, n_tp)
    done = []
    rows_tp = tokens.shape[0]

    def sum_tp(k, left, right):
        batch = n_tp * rows_tp
        values = left[...].astype(F32).reshape(batch, left.shape[2]).astype(BF16)
        product = jnp.dot(values, right[...], preferred_element_type=F32)
        product = product.reshape(n_tp, rows_tp, product.shape[1])
        t_acc[...] = product
        t_send_buf[k] = product.astype(BF16)
        copies = exchange_start(
            lambda peer: t_send_buf.at[k, peer], t_recv_buf.at[k], ts.at[k], tr.at[k], "tp", n_tp
        )
        total = t_acc[tp]
        for off in range(1, n_tp):
            copies[off - 1].wait_recv()
            total = total + t_recv_buf[k, lax.rem(tp + n_tp - off, n_tp)].astype(F32)
        done.extend(copies)
        return total

    done.extend(gather_kv(gated, g_all, gs, gr, gfs, gfr, n_kv))
    loads[0].wait()
    attended = sum_tp(0, g_all, v_out)
    r_own[...] = (tokens[...].astype(F32) + attended).astype(BF16)
    copies = exchange_start(lambda peer: r_own, r_all, ts.at[2], tr.at[2], "tp", n_tp)
    r_all[tp] = r_own[...]
    for copy in copies:
        copy.wait_recv()
    done.extend(copies)
    values = r_all[...].astype(F32).reshape(n_tp * rows_tp, tokens.shape[1])
    normed = (values * gain[...]).astype(BF16)
    scatter = Scatter(scatter_refs, n_kv)
    cols = v_ffn.shape[2]
    step = cols // chunks
    tile = next(t for t in (640, 512, 256, 128) if step % t == 0)
    order = [(w, h) for h in range(chunks) for w in range(2)]
    loads[1].wait()
    loads[2].wait()
    squares = None
    for c, (w, h) in enumerate(order):
        for at in range(0, step, tile):
            product = jnp.dot(
                normed, v_ffn[w, :, pl.ds(h * step + at, tile)], preferred_element_type=F32
            )
            scatter.put(c, pl.ds(at, tile), product)
        scatter.send_pair(c)
        if c > 0:
            scatter.send_rest(c - 1)
        if c == 0:
            squares = squares_start(values, square_refs, n_kv)
    scatter.send_rest(2 * chunks - 1)
    factor = squares_factor(squares, square_refs, n_kv, width)
    done.extend(squares)
    for h in range(chunks):
        gate = scatter.total(2 * h) * factor
        up = scatter.total(2 * h + 1) * factor
        h_own[:, h * step : (h + 1) * step] = (jax.nn.silu(gate) * up).astype(BF16)
    done.extend(gather_kv(h_own, h_all, hs, hr, hfs, hfr, n_kv))
    loads[3].wait()
    down = sum_tp(1, h_all, v_down)
    out[...] = (r_own[...].astype(F32) + down).astype(BF16)
    for copy in done:
        copy.wait_send()
    scatter.close()


def body(
    n_kv,
    n_tp,
    tokens,
    state,
    mix_gain,
    q_weight,
    forget_weight,
    input_weight,
    gate_weight,
    lower_bound,
    head_gain,
    out_weight,
    ffn_gain,
    ffn_gate,
    ffn_up,
    ffn_down,
):
    rows_tp, feats = tokens.shape
    width = feats * n_kv
    rows_kv, heads, size = state.shape[:3]
    cols = q_weight.shape[1]
    ff = ffn_gate.shape[1]
    dma = pltpu.SemaphoreType.DMA
    sums = pl.pallas_call(
        functools.partial(mixer_in, n_kv, n_tp, width),
        out_shape=jax.ShapeDtypeStruct((rows_kv, 4 * cols), F32),
        in_specs=[VMEM, VMEM, HBM, HBM, HBM, HBM],
        out_specs=VMEM,
        scratch_shapes=[
            pltpu.VMEM((n_tp, rows_tp, feats), BF16),
            pltpu.VMEM((4, feats, cols), BF16),
            *scatter_scratch(4, n_kv, rows_kv, cols),
            *squares_scratch(n_kv, rows_kv),
            dma((4,)),
            dma((n_tp,)),
            dma((n_tp,)),
        ],
        compiler_params=pltpu.CompilerParams(
            collective_id=0, has_side_effects=True, vmem_limit_bytes=min(60 * MIB, 67043328 - state.size * 4 - MIB)
        ),
        cost_estimate=pl.CostEstimate(
            flops=32 * n_tp * rows_tp * feats * 4 * cols,
            bytes_accessed=16 * feats * 4 * cols,
            transcendentals=0,
        ),
        name="mixer_in",
    )(tokens, mix_gain[None, :], q_weight, forget_weight, input_weight, gate_weight)

    def part(i):
        return pl.BlockSpec((rows_kv, size), lambda h: (0, i * heads + h))

    state_block = pl.BlockSpec((rows_kv, 1, size, size), lambda h: (0, h, 0, 0))
    new_state, gated = pl.pallas_call(
        state_step,
        out_shape=(
            jax.ShapeDtypeStruct(state.shape, F32),
            jax.ShapeDtypeStruct((rows_kv, cols), BF16),
        ),
        grid=(heads,),
        in_specs=[
            part(0),
            part(1),
            part(2),
            part(3),
            pl.BlockSpec((1, size), lambda h: (0, h)),
            pl.BlockSpec((1, size), lambda h: (0, 0)),
            state_block,
        ],
        out_specs=(state_block, pl.BlockSpec((rows_kv, size), lambda h: (0, h))),
        scratch_shapes=[pltpu.VMEM((rows_kv, size), F32)],
        compiler_params=pltpu.CompilerParams(dimension_semantics=("arbitrary",), vmem_limit_bytes=16 * MIB),
        cost_estimate=pl.CostEstimate(
            flops=6 * rows_kv * heads * size * size,
            bytes_accessed=8 * rows_kv * heads * size * size,
            transcendentals=0,
        ),
        name="state_step",
    )(sums, sums, sums, sums, lower_bound[None, :], head_gain[None, :], state)

    half = n_kv // 2
    chunks = 2 if ff % (2 * LANES) == 0 else 1
    layer_out = pl.pallas_call(
        functools.partial(rest_of_layer, n_kv, n_tp, width, chunks),
        out_shape=jax.ShapeDtypeStruct(tokens.shape, BF16),
        in_specs=[VMEM, VMEM, VMEM, HBM, HBM, HBM, HBM],
        out_specs=VMEM,
        scratch_shapes=[
            pltpu.VMEM((cols, feats), BF16),
            pltpu.VMEM((2, feats, ff), BF16),
            pltpu.VMEM((ff, feats), BF16),
            pltpu.VMEM((n_kv, rows_kv, cols), BF16),
            pltpu.VMEM((rows_kv, ff), BF16),
            pltpu.VMEM((n_kv, rows_kv, ff), BF16),
            pltpu.VMEM((n_tp, rows_tp, feats), F32),
            pltpu.VMEM((2, n_tp, rows_tp, feats), BF16),
            pltpu.VMEM((2, n_tp, rows_tp, feats), BF16),
            pltpu.VMEM((rows_tp, feats), BF16),
            pltpu.VMEM((n_tp, rows_tp, feats), BF16),
            *scatter_scratch(2 * chunks, n_kv, rows_kv, ff // chunks),
            *squares_scratch(n_kv, rows_kv),
            dma((4,)),
            *[dma((half,)) for _ in range(8)],
            dma((3, n_tp)),
            dma((3, n_tp)),
        ],
        compiler_params=pltpu.CompilerParams(collective_id=1, has_side_effects=True),
        name="rest_of_layer",
    )(tokens, gated, ffn_gain[None, :], out_weight, ffn_gate, ffn_up, ffn_down)
    return (layer_out, new_state)


def solution(mesh):
    in_specs = (
        P("tp", "kv"),
        P("kv", "tp", None, None),
        P("kv"),
        P("kv", "tp"),
        P("kv", "tp"),
        P("kv", "tp"),
        P("kv", "tp"),
        P("tp"),
        P(),
        P("tp", "kv"),
        P("kv"),
        P("kv", "tp"),
        P("kv", "tp"),
        P("tp", "kv"),
    )
    out_specs = (P("tp", "kv"), P("kv", "tp", None, None))
    step = functools.partial(body, mesh.shape["kv"], mesh.shape["tp"])
    return jax.shard_map(step, mesh=mesh, in_specs=in_specs, out_specs=out_specs, check_vma=False)
```
